768 devices in a mesh: fs: 24 (over z, core), tp: 32 (over y, x).
Axes of the slice: x: 4, y: 8, z: 12, core: 2. Of those that a mesh axis runs over, the one named last changes fastest.
Arguments:
- saved_input: bfloat16 [24576, 2304], P('fs', 'tp'), may hold values from -6 to 6
- cot_forget: bfloat16 [24576, 2304], P('fs', 'tp'), may hold values from -0.038085938 to 0.038085938
- cot_value: bfloat16 [24576, 2304], P('fs', 'tp'), may hold values from -0.038085938 to 0.038085938
- basis_forget: bfloat16 [2304, 288], replicated, may hold values from -2 to 2
- basis_value: bfloat16 [2304, 288], replicated, may hold values from -2 to 2
- first_forget: float32 [288, 2304], P('fs', 'tp'), may hold values from -180 to 180
- first_value: float32 [288, 2304], P('fs', 'tp'), may hold values from -180 to 180
- second_forget: float32 [288, 2304], P('fs', 'tp'), may hold values from 0.1 to 1
- second_value: float32 [288, 2304], P('fs', 'tp'), may hold values from 0.1 to 1
- weight_forget: float32 [2304, 2304], P('fs', 'tp'), may hold values from -0.125 to 0.125
- weight_value: float32 [2304, 2304], P('fs', 'tp'), may hold values from -0.125 to 0.125
Outputs:
- new_first_forget: float32 [288, 2304], P('fs', 'tp')
- new_second_forget: float32 [288, 2304], P('fs', 'tp')
- step_forget: float32 [2304, 2304], P('fs', 'tp')
- new_weight_forget: float32 [2304, 2304], P('fs', 'tp')
- copy_forget: bfloat16 [2304, 2304], P(None, 'tp')
- new_first_value: float32 [288, 2304], P('fs', 'tp')
- new_second_value: float32 [288, 2304], P('fs', 'tp')
- step_value: float32 [2304, 2304], P('fs', 'tp')
- new_weight_value: float32 [2304, 2304], P('fs', 'tp')
- copy_value: bfloat16 [2304, 2304], P(None, 'tp')
The draws below stay inside these ranges and needn't reach their ends.
All inputs are finite; a program needn't handle non-finite values.
Results may differ from the reference program's by a relative error of at most 0.0042.
Values may be sent and summed in bfloat16 or wider, within the bound.
No kernel may reach another device: no remote copies, remote signals or barrier semaphores. Data moves between devices by JAX's collectives and lax.ppermute only.
A program may use at most 32 MiB of HBM per device.

```python
import math
import jax
import jax.numpy as jnp
from jax import lax

D = 2304
RANK = 288
TOKENS = 24576


def rising_draw(key, row_count, col_count, col_span):
    raw_values = jnp.clip(jax.random.normal(key, (row_count, col_count), jnp.float32), -4.0, 4.0)
    stretch = math.log(3.0)
    row_pos = jnp.arange(row_count, dtype=jnp.float32) / max(row_count - 1, 1)
    col_pos = jnp.arange(col_count, dtype=jnp.float32) / max(col_count - 1, 1)
    factor = jnp.exp(stretch * (row_pos[:, None] + col_span * col_pos[None, :]))
    return raw_values * factor


def draw_basis_forget(key, part):
    return (rising_draw(jax.random.fold_in(key, 11), D, RANK, 0.0) * D ** (-0.5)).astype(jnp.bfloat16)


def draw_basis_value(key, part):
    return (rising_draw(jax.random.fold_in(key, 12), D, RANK, 0.0) * D ** (-0.5)).astype(jnp.bfloat16)


def draw_first_forget(key, part):
    return rising_draw(jax.random.fold_in(key, 13), RANK, D, 1.0)


def draw_first_value(key, part):
    return rising_draw(jax.random.fold_in(key, 14), RANK, D, 1.0)


def levels(own_key, dims, split, least, largest):
    loudness = 1.0
    for position, blocks in split:
        draws = jax.random.uniform(jax.random.fold_in(jax.random.fold_in(own_key, 6), position), (blocks,), jnp.float32, least / len(split), largest / len(split))
        loudness = loudness * jnp.repeat(jnp.exp(draws), dims[position] // blocks).reshape((-1,) + (1,) * (len(dims) - 1 - position))
    return loudness


def centred(rng, extent, scale, reach, shards=(), kind=jnp.bfloat16):
    entries = scale * jax.random.normal(rng, extent, jnp.float32)
    if shards:
        entries = entries * levels(rng, extent, shards, -0.22, 0.18)
    return jnp.clip(entries, -reach, reach).astype(kind)


def setup_inputs(seed: int = 0) -> dict:
    keys = jax.random.split(jax.random.key(seed), 12)
    return {
        "saved_input": centred(keys[0], (TOKENS, D), 1.0, 6.0, ((0, 24), (1, 32))),
        "cot_forget": centred(keys[1], (TOKENS, D), (TOKENS ** -0.5), 0.038085938, ((0, 24), (1, 32))),
        "cot_value": centred(keys[2], (TOKENS, D), (TOKENS ** -0.5), 0.038085938, ((0, 24), (1, 32))),
        "basis_forget": draw_basis_forget(jax.random.fold_in(keys[11], 71), 0),
        "basis_value": draw_basis_value(jax.random.fold_in(keys[11], 71), 0),
        "first_forget": draw_first_forget(jax.random.fold_in(keys[11], 71), 0),
        "first_value": draw_first_value(jax.random.fold_in(keys[11], 71), 0),
        "second_forget": jnp.clip(jnp.exp(math.log(1.0) - 2.3025851 * jax.random.uniform(keys[7], (RANK, D), jnp.float32) ** levels(keys[7], (RANK, D), ((0, 24), (1, 32)), -0.2, 0.2)), 0.1, 1.0),
        "second_value": jnp.clip(jnp.exp(math.log(1.0) - 2.3025851 * jax.random.uniform(keys[8], (RANK, D), jnp.float32) ** levels(keys[8], (RANK, D), ((0, 24), (1, 32)), -0.2, 0.2)), 0.1, 1.0),
        "weight_forget": centred(keys[9], (D, D), D ** -0.5, 0.125, ((0, 24), (1, 32)), jnp.float32),
        "weight_value": centred(keys[10], (D, D), D ** -0.5, 0.125, ((0, 24), (1, 32)), jnp.float32),
    }


beta_one = 0.8
beta_two = 0.9
rate = 0.02
epsilon = 1e-06

def project(saved_input, cotangent, basis):
    inputs_basis = jnp.dot(saved_input.astype(jnp.float32), basis.astype(jnp.float32), precision=lax.Precision.HIGHEST)
    return jnp.dot(inputs_basis.T, cotangent.astype(jnp.float32), precision=lax.Precision.HIGHEST)

def advance(projected, first, second, basis, weight):
    new_first = beta_one * first + (1.0 - beta_one) * projected
    new_second = beta_two * second + (1.0 - beta_two) * projected * projected
    direction = (new_first / jnp.sqrt(new_second)).astype(jnp.bfloat16)
    update = jnp.dot(basis.astype(jnp.float32), direction.astype(jnp.float32), precision=lax.Precision.HIGHEST)
    mean_square = jnp.mean(update * update)
    step = update / jnp.sqrt(mean_square + epsilon)
    new_weight = weight - rate * step
    return (new_first, new_second, step, new_weight, new_weight.astype(jnp.bfloat16))

def reference(saved_input, cot_forget, cot_value, basis_forget, basis_value, first_forget, first_value, second_forget, second_value, weight_forget, weight_value):
    proj_forget = project(saved_input, cot_forget, basis_forget)
    proj_value = project(saved_input, cot_value, basis_value)
    out_forget = advance(proj_forget, first_forget, second_forget, basis_forget, weight_forget)
    out_value = advance(proj_value, first_value, second_value, basis_value, weight_value)
    return (out_forget[0], out_forget[1], out_forget[2], out_forget[3], out_forget[4], out_value[0], out_value[1], out_value[2], out_value[3], out_value[4])
```

```python
import jax
import jax.numpy as jnp
from jax import lax
from jax.sharding import Mesh
from jax.sharding import PartitionSpec as P

D = 2304
RANK = 288
FS = ("fs_0", "fs_1")
TP = ("tp_0", "tp_1")
TP_X_FIRST = ("tp_1", "tp_0")

beta_one = 0.8
beta_two = 0.9
rate = 0.02
epsilon = 1e-06


def exchanged(blocks, axes):
    return lax.all_to_all(blocks, axes, 0, 0, tiled=True)


def spread(array, axes):
    return exchanged(jnp.broadcast_to(array[None], (lax.axis_size(axes), *array.shape)), axes)


def over_tokens(left, right):
    return lax.dot_general(
        left, right, (((0,), (0,)), ((), ())), preferred_element_type=jnp.float32
    )


def moments(projected, first, second):
    new_first = beta_one * first + (1.0 - beta_one) * projected
    new_second = beta_two * second + (1.0 - beta_two) * projected * projected
    direction = (new_first / jnp.sqrt(new_second)).astype(jnp.bfloat16)
    return (new_first, new_second, direction)


def body(
    saved_input,
    cot_forget,
    cot_value,
    basis_forget,
    basis_value,
    first_forget,
    first_value,
    second_forget,
    second_value,
    weight_forget,
    weight_value,
):
    tokens, width = saved_input.shape
    ny, nx = lax.axis_size("tp_0"), lax.axis_size("tp_1")
    nt, nf = nx * ny, lax.axis_size(FS)
    own_rows = weight_forget.shape[0]
    own_tokens = tokens // nt

    all_weights = lax.all_gather(
        jnp.concatenate([weight_forget, weight_value], axis=1), FS, axis=0, tiled=True
    )

    mine = exchanged(saved_input.reshape(nt, own_tokens, width), TP_X_FIRST)
    mine = mine.reshape(nx, ny, own_tokens, width).transpose(2, 1, 0, 3).reshape(own_tokens, D)
    reduced = jnp.concatenate(
        [
            jnp.dot(mine, basis_forget, preferred_element_type=jnp.float32),
            jnp.dot(mine, basis_value, preferred_element_type=jnp.float32),
        ],
        axis=1,
    ).astype(jnp.bfloat16)
    reduced = spread(reduced, "tp_0").reshape(ny * own_tokens, 2 * RANK)
    reduced = spread(reduced, "tp_1").reshape(tokens, 2 * RANK)

    partial = jnp.concatenate(
        [over_tokens(reduced[:, :RANK], cot_forget), over_tokens(reduced[:, RANK:], cot_value)],
        axis=1,
    )
    projected = jnp.sum(exchanged(partial.reshape(nf, RANK // nf, 2 * width), FS), axis=0)
    new_first_forget, new_second_forget, direction_forget = moments(
        projected[:, :width], first_forget, second_forget
    )
    new_first_value, new_second_value, direction_value = moments(
        projected[:, width:], first_value, second_value
    )
    directions = spread(
        jnp.concatenate([direction_forget, direction_value], axis=1), FS
    ).reshape(RANK, 2 * width)
    update_forget = jnp.dot(
        basis_forget, directions[:, :width], preferred_element_type=jnp.float32
    )
    update_value = jnp.dot(
        basis_value, directions[:, width:], preferred_element_type=jnp.float32
    )
    squares = jnp.stack(
        [jnp.sum(update_forget * update_forget), jnp.sum(update_value * update_value)]
    )
    squares = jnp.sum(spread(jnp.broadcast_to(squares[:, None], (2, 128))[:, None].reshape(1, 256), TP), axis=0)
    entries = float(D * D)
    scale_forget = 1.0 / jnp.sqrt(squares[0, 0] / entries + epsilon)
    scale_value = 1.0 / jnp.sqrt(squares[0, 128] / entries + epsilon)
    row_start = lax.axis_index(FS) * own_rows

    def finished(update, scale, weight, whole_weight):
        step = lax.dynamic_slice_in_dim(update, row_start, own_rows, 0) * scale
        copy = (whole_weight - rate * (update * scale)).astype(jnp.bfloat16)
        return (step, weight - rate * step, copy)

    step_forget, new_weight_forget, copy_forget = finished(
        update_forget, scale_forget, weight_forget, all_weights[:, :width]
    )
    step_value, new_weight_value, copy_value = finished(
        update_value, scale_value, weight_value, all_weights[:, width:]
    )
    return (
        new_first_forget,
        new_second_forget,
        step_forget,
        new_weight_forget,
        copy_forget,
        new_first_value,
        new_second_value,
        step_value,
        new_weight_value,
        copy_value,
    )


def solution(mesh):
    split = Mesh(mesh.devices.reshape(12, 2, 8, 4), ("fs_0", "fs_1", "tp_0", "tp_1"))
    own = P(FS, TP)
    columns = P(None, TP)
    return jax.shard_map(
        body,
        mesh=split,
        in_specs=(own, own, own, P(), P(), own, own, own, own, own, own),
        out_specs=(own, own, own, own, columns) * 2,
        check_vma=False,
    )
```
